32 devices in a mesh: fs: 4 (over y, x), tp: 8 (over z, core).
Axes of the slice: x: 2, y: 2, z: 4, core: 2. Of those that a mesh axis runs over, the one named last changes fastest.
Arguments:
- later_tokens: bfloat16 [1792, 2048], P(('fs', 'tp')), may hold values from -6 to 6
- earlier_tokens: bfloat16 [1792, 2048], P(('fs', 'tp')), may hold values from -6 to 6
- earlier_cotangent: bfloat16 [1792, 2048], P(('fs', 'tp')), may hold values from -6 to 6
- gate_weight: bfloat16 [2048, 5632], P('fs', 'tp'), may hold values from -0.125 to 0.125
- up_weight: bfloat16 [2048, 5632], P('fs', 'tp'), may hold values from -0.125 to 0.125
- down_weight: bfloat16 [5632, 2048], P('tp', 'fs'), may hold values from -0.078125 to 0.078125
- gate_sum: float32 [2048, 5632], P('fs', 'tp'), may hold values from -48 to 48
- up_sum: float32 [2048, 5632], P('fs', 'tp'), may hold values from -48 to 48
- down_sum: float32 [5632, 2048], P('tp', 'fs'), may hold values from -48 to 48
Outputs:
- later_output: bfloat16 [1792, 2048], P(('fs', 'tp'))
- earlier_grad: bfloat16 [1792, 2048], P(('fs', 'tp'))
- gate_total: float32 [2048, 5632], P('fs', 'tp')
- up_total: float32 [2048, 5632], P('fs', 'tp')
- down_total: float32 [5632, 2048], P('tp', 'fs')
The draws below stay inside these ranges and needn't reach their ends.
All inputs are finite; a program needn't handle non-finite values.
Results may differ from the reference program's by a relative error of at most 0.018.
Values may be sent and summed in bfloat16 or wider, within the bound.
A program may use at most 128 MiB of HBM per device.

```python
import jax
import jax.numpy as jnp
from jax import lax

D = 2048
FF = 5632
TOKENS = 1792
N_TP = 8


def raised(entries, key, source, target, shards_of, factor):
    owner, partner = [(jnp.arange(entries.shape[dim]) // (entries.shape[dim] // shards_of)).reshape([-1 if axis == dim else 1 for axis in range(entries.ndim)]) for dim in (source, target)]
    chosen = jax.random.permutation(key, shards_of)[partner]
    strong = (owner == chosen) | (owner == (partner + shards_of // 2) % shards_of)
    return jnp.where(strong, factor * entries, entries)


def levels(own_key, extent, split, low, high):
    level, own = 1.0, jax.random.fold_in(own_key, 6)
    for dim, shards_of in split:
        steps = jnp.exp(jax.random.uniform(jax.random.fold_in(own, dim), (shards_of,), jnp.float32, low / len(split), high / len(split)))
        level = level * jnp.repeat(steps, extent[dim] // shards_of).reshape([-1 if axis == dim else 1 for axis in range(len(extent))])
    return level


def centred(rng, shape, deviation, limit, cuts=(), kind=jnp.bfloat16):
    values = deviation * jax.random.normal(rng, shape, jnp.float32)
    if cuts:
        values = values * levels(rng, shape, cuts, -0.22, 0.18)
    return jnp.clip(values, -limit, limit).astype(kind)


def heavy_noise(own_key, dims, spread, reach, shards, heavy, held_as=jnp.bfloat16):
    drawn = spread * jax.random.normal(own_key, dims, jnp.float32)
    if shards:
        drawn = drawn * levels(own_key, dims, shards, -0.22, 0.18)
    return jnp.clip(raised(drawn, jax.random.fold_in(own_key, 3), *heavy), -reach, reach).astype(held_as)


def setup_inputs(seed: int = 0) -> dict:
    key_of = jax.random.split(jax.random.key(seed), 10)
    return {
        "later_tokens": centred(key_of[0], (TOKENS, D), 1.0, 6.0, ((0, 32),)),
        "earlier_tokens": centred(key_of[1], (TOKENS, D), 1.0, 6.0, ((0, 32),)),
        "earlier_cotangent": heavy_noise(key_of[2], (TOKENS, D), 1.0, 6.0, ((0, 32),), (0, 1, 32, 2.75)),
        "gate_weight": centred(key_of[3], (D, FF), D ** -0.5, 0.125, ((0, 4), (1, 8))),
        "up_weight": centred(key_of[4], (D, FF), D ** -0.5, 0.125, ((0, 4), (1, 8))),
        "down_weight": centred(key_of[5], (FF, D), FF ** -0.5, 0.078125, ((0, 8), (1, 4))),
        "gate_sum": centred(key_of[6], (D, FF), 8.0, 48.0, ((0, 4), (1, 8)), jnp.float32),
        "up_sum": centred(key_of[7], (D, FF), 8.0, 48.0, ((0, 4), (1, 8)), jnp.float32),
        "down_sum": centred(key_of[8], (FF, D), 8.0, 48.0, ((0, 8), (1, 4)), jnp.float32),
    }


def blocked_sum(lefts, rights, rows):
    def step(total, pair):
        lhs, rhs = pair
        part = jnp.zeros((rows, D), jnp.float32)
        for left, right in zip(lhs, rhs):
            part = part + jnp.dot(left, right, preferred_element_type=jnp.float32)
        part = lax.optimization_barrier(part.astype(jnp.bfloat16))
        return total + part.astype(jnp.float32), None

    total, unused = lax.scan(step, jnp.zeros((rows, D), jnp.float32), (lefts, rights))
    return total.astype(jnp.bfloat16)


def split_columns(matrix):
    rows = matrix.shape[0]
    return matrix.reshape(rows, N_TP, FF // N_TP).transpose(1, 0, 2)


def split_rows(matrix):
    return matrix.reshape(N_TP, FF // N_TP, matrix.shape[1])


def reference(later_tokens, earlier_tokens, earlier_cotangent, gate_weight, up_weight, down_weight, gate_sum, up_sum, down_sum):
    rows = later_tokens.shape[0]
    later_gate = jnp.dot(later_tokens, gate_weight, preferred_element_type=jnp.float32)
    later_up = jnp.dot(later_tokens, up_weight, preferred_element_type=jnp.float32)
    later_hidden = (jax.nn.silu(later_gate) * later_up).astype(jnp.bfloat16)
    later_output = blocked_sum((split_columns(later_hidden),), (split_rows(down_weight),), rows)

    earlier_gate = jnp.dot(earlier_tokens, gate_weight, preferred_element_type=jnp.float32)
    earlier_up = jnp.dot(earlier_tokens, up_weight, preferred_element_type=jnp.float32)
    sigmoid_gate = jax.nn.sigmoid(earlier_gate)
    earlier_act = earlier_gate * sigmoid_gate
    earlier_hidden = (earlier_act * earlier_up).astype(jnp.bfloat16)
    hidden_grad = jnp.dot(earlier_cotangent, down_weight.T, preferred_element_type=jnp.float32)
    slope = sigmoid_gate * (1.0 + earlier_gate * (1.0 - sigmoid_gate))
    gate_grad = (hidden_grad * earlier_up * slope).astype(jnp.bfloat16)
    up_grad = (hidden_grad * earlier_act).astype(jnp.bfloat16)
    earlier_grad = blocked_sum((split_columns(gate_grad), split_columns(up_grad)),
                               (split_rows(gate_weight.T), split_rows(up_weight.T)), rows)

    gate_total = gate_sum + jnp.dot(earlier_tokens.T, gate_grad, preferred_element_type=jnp.float32)
    up_total = up_sum + jnp.dot(earlier_tokens.T, up_grad, preferred_element_type=jnp.float32)
    down_total = down_sum + jnp.dot(earlier_hidden.T, earlier_cotangent, preferred_element_type=jnp.float32)
    return later_output, earlier_grad, gate_total, up_total, down_total
```

```python
import jax
import jax.numpy as jnp
from jax import lax
from jax.sharding import PartitionSpec as P


def transposed_dot(left, right):
    return lax.dot_general(
        left, right, (((1,), (1,)), ((), ())), preferred_element_type=jnp.float32
    )


def rows_dot(left, right):
    return lax.dot_general(
        left, right, (((0,), (0,)), ((), ())), preferred_element_type=jnp.float32
    )


def dot(left, right):
    return jnp.dot(left, right, preferred_element_type=jnp.float32)


def swap(value, mask):
    return lax.ppermute(value, "fs", [(i, i ^ mask) for i in range(4)])


def after(value, *first):
    return lax.optimization_barrier((value, *first))[0]


def halves(value, axis=0):
    return jnp.split(value, 2, axis=axis)


def near(weight):
    return swap(weight, 1), swap(weight, 2)


def far(by_x, by_y):
    return swap(halves(by_x)[0], 2), swap(halves(by_y)[1], 1)


def scatter_start(blocks):
    one, two, three = (halves(b) for b in blocks[1:])
    return (swap(one[0], 1), swap(three[0], 1), swap(two[1], 2), swap(three[1], 2))


def scatter_end(blocks, got):
    own, one, two = (halves(b) for b in blocks[:3])
    f32 = jnp.float32
    along_y = swap((two[0].astype(f32) + got[1].astype(f32)).astype(jnp.bfloat16), 2)
    along_x = swap((one[1].astype(f32) + got[3].astype(f32)).astype(jnp.bfloat16), 1)
    first = own[0].astype(f32) + got[0].astype(f32) + along_y.astype(f32)
    second = own[1].astype(f32) + got[2].astype(f32) + along_x.astype(f32)
    return jnp.concatenate([first, second], axis=0)


def silu_parts(gate):
    s = jax.nn.sigmoid(gate)
    return s, gate * s


def reorder(value, me):
    size = value.shape[1] // 4
    return jnp.concatenate(
        [lax.dynamic_slice_in_dim(value, (me ^ j) * size, size, axis=1) for j in range(4)],
        axis=1,
    )


def tp_gather(value):
    return lax.all_gather(value, "tp", axis=0, tiled=True)


def tp_scatter(value):
    return lax.psum_scatter(value, "tp", scatter_dimension=0, tiled=True)


def body4(
    later_tokens,
    earlier_tokens,
    earlier_cotangent,
    gate_weight,
    up_weight,
    down_weight,
    gate_sum,
    up_sum,
    down_sum,
):
    bf16 = jnp.bfloat16
    me = lax.axis_index("fs")
    e_tok = tp_gather(reorder(earlier_tokens, me))
    e_cot = tp_gather(reorder(earlier_cotangent, me))
    l_tok = tp_gather(reorder(later_tokens, me))

    g1, g2 = near(gate_weight)
    u1, u2 = near(up_weight)
    g3 = far(g1, g2)
    d1, d2 = near(after(down_weight, g1, g2))
    u3 = far(u1, u2)
    d3 = far(d1, d2)
    gate_w = jnp.concatenate([gate_weight, g1, g2, *g3], axis=0)
    up_w = jnp.concatenate([up_weight, u1, u2, *u3], axis=0)
    down_w = jnp.concatenate(
        [down_weight, d1, d2, jnp.concatenate(d3, axis=0)], axis=1
    )

    earlier_gate = dot(e_tok, gate_w)
    earlier_up = dot(e_tok, up_w)
    s, act = silu_parts(earlier_gate)
    earlier_hidden = (act * earlier_up).astype(bf16)

    size = e_cot.shape[1] // 4
    down_blocks = [
        rows_dot(earlier_hidden, e_cot[:, j * size : (j + 1) * size]).astype(bf16)
        for j in range(4)
    ]
    down_got = scatter_start(down_blocks)

    hidden_grad = transposed_dot(e_cot, down_w)
    slope = s * (1.0 + earlier_gate * (1.0 - s))
    gate_grad = (hidden_grad * earlier_up * slope).astype(bf16)
    up_grad = (hidden_grad * act).astype(bf16)

    gate_blocks = [
        rows_dot(e_tok[:, j * size : (j + 1) * size], gate_grad).astype(bf16) for j in range(4)
    ]
    up_blocks = [
        rows_dot(e_tok[:, j * size : (j + 1) * size], up_grad).astype(bf16) for j in range(4)
    ]
    gate_got = scatter_start(gate_blocks)
    up_got = scatter_start(up_blocks)

    later_hidden = (jax.nn.silu(dot(l_tok, gate_w)) * dot(l_tok, up_w)).astype(bf16)
    later_output = tp_scatter(dot(later_hidden, down_w).astype(bf16))
    earlier_grad = tp_scatter(
        (transposed_dot(gate_grad, gate_w) + transposed_dot(up_grad, up_w)).astype(bf16)
    )
    down_total = down_sum + scatter_end(down_blocks, down_got)
    gate_total = gate_sum + scatter_end(gate_blocks, gate_got)
    up_total = up_sum + scatter_end(up_blocks, up_got)
    return (reorder(later_output, me), reorder(earlier_grad, me), gate_total, up_total, down_total)


def body(
    later_tokens,
    earlier_tokens,
    earlier_cotangent,
    gate_weight,
    up_weight,
    down_weight,
    gate_sum,
    up_sum,
    down_sum,
):
    width = gate_weight.shape[1]
    gate_w, up_w, down_w = (
        lax.all_gather(gate_weight, "fs", axis=0, tiled=True),
        lax.all_gather(up_weight, "fs", axis=0, tiled=True),
        lax.all_gather(down_weight, "fs", axis=1, tiled=True),
    )
    piece = tp_gather(later_tokens)
    later_hidden = (jax.nn.silu(dot(piece, gate_w)) * dot(piece, up_w)).astype(jnp.bfloat16)
    later_output = tp_scatter(dot(later_hidden, down_w).astype(jnp.bfloat16))
    group_tokens, group_cotangent = tp_gather(earlier_tokens), tp_gather(earlier_cotangent)
    earlier_gate = dot(group_tokens, gate_w)
    earlier_up = dot(group_tokens, up_w)
    s, act = silu_parts(earlier_gate)
    earlier_hidden = (act * earlier_up).astype(jnp.bfloat16)
    hidden_grad = transposed_dot(group_cotangent, down_w)
    slope = s * (1.0 + earlier_gate * (1.0 - s))
    gate_grad = (hidden_grad * earlier_up * slope).astype(jnp.bfloat16)
    up_grad = (hidden_grad * act).astype(jnp.bfloat16)
    earlier_grad = tp_scatter(
        (transposed_dot(gate_grad, gate_w) + transposed_dot(up_grad, up_w)).astype(jnp.bfloat16)
    )
    summed = lax.psum_scatter(
        jnp.concatenate(
            [
                rows_dot(group_tokens, gate_grad),
                rows_dot(group_tokens, up_grad),
                rows_dot(group_cotangent, earlier_hidden),
            ],
            axis=1,
        ).astype(jnp.bfloat16),
        "fs",
        scatter_dimension=0,
        tiled=True,
    ).astype(jnp.float32)
    gate_total = gate_sum + summed[:, :width]
    up_total = up_sum + summed[:, width : 2 * width]
    down_total = down_sum + summed[:, 2 * width :].T
    return (later_output, earlier_grad, gate_total, up_total, down_total)


def solution(mesh):
    return jax.shard_map(
        body4 if mesh.shape["fs"] == 4 else body,
        mesh=mesh,
        in_specs=(
            P(("fs", "tp"), None),
            P(("fs", "tp"), None),
            P(("fs", "tp"), None),
            P("fs", "tp"),
            P("fs", "tp"),
            P("tp", "fs"),
            P("fs", "tp"),
            P("fs", "tp"),
            P("tp", "fs"),
        ),
        out_specs=(
            P(("fs", "tp"), None),
            P(("fs", "tp"), None),
            P("fs", "tp"),
            P("fs", "tp"),
            P("tp", "fs"),
        ),
        check_vma=False,
    )
```

```python
import functools

import jax
import jax.numpy as jnp
from jax import lax
from jax.sharding import PartitionSpec as P


def transposed_dot(left, right):
    return lax.dot_general(
        left, right, (((1,), (1,)), ((), ())), preferred_element_type=jnp.float32
    )


def rows_dot(left, right):
    return lax.dot_general(
        left, right, (((0,), (0,)), ((), ())), preferred_element_type=jnp.float32
    )


def dot(left, right):
    return jnp.dot(left, right, preferred_element_type=jnp.float32)


def swap(value, mask):
    return lax.ppermute(value, "fs", [(i, i ^ mask) for i in range(4)])


def after(value, *first):
    return lax.optimization_barrier((value, *first))[0]


def halves(value, axis=0):
    return jnp.split(value, 2, axis=axis)


def near(weight):
    return swap(weight, 1), swap(weight, 2)


def far(by_x, by_y):
    return swap(halves(by_x)[0], 2), swap(halves(by_y)[1], 1)


def scatter_start(blocks):
    one, two, three = (halves(b) for b in blocks[1:])
    return (swap(one[0], 1), swap(three[0], 1), swap(two[1], 2), swap(three[1], 2))


def scatter_end(blocks, got):
    own, one, two = (halves(b) for b in blocks[:3])
    f32 = jnp.float32
    along_y = swap((two[0].astype(f32) + got[1].astype(f32)).astype(jnp.bfloat16), 2)
    along_x = swap((one[1].astype(f32) + got[3].astype(f32)).astype(jnp.bfloat16), 1)
    first = own[0].astype(f32) + got[0].astype(f32) + along_y.astype(f32)
    second = own[1].astype(f32) + got[2].astype(f32) + along_x.astype(f32)
    return jnp.concatenate([first, second], axis=0)


def silu_parts(gate):
    s = jax.nn.sigmoid(gate)
    return s, gate * s


def reorder(value, me):
    size = value.shape[1] // 4
    return jnp.concatenate(
        [lax.dynamic_slice_in_dim(value, (me ^ j) * size, size, axis=1) for j in range(4)],
        axis=1,
    )


def summed(one, two):
    return (one.astype(jnp.float32) + two.astype(jnp.float32)).astype(jnp.bfloat16)


def shift(value, step, size):
    return lax.ppermute(value, "tp", [(i, (i + 2 * step) % size) for i in range(size)])


def flip(value, size):
    return lax.ppermute(value, "tp", [(i, i ^ 1) for i in range(size)])


def group_scatter(value, size):
    rows = value.shape[0] // size
    at = lax.axis_index("tp")
    core, z, chips = at % 2, at // 2, size // 2
    value = value.reshape(chips, 2, rows, value.shape[1])
    mine = lax.dynamic_slice_in_dim(value, core, 1, axis=1)[:, 0]
    other = lax.dynamic_slice_in_dim(value, 1 - core, 1, axis=1)[:, 0]
    pair = summed(mine, flip(other, size))
    total = lax.dynamic_slice_in_dim(pair, z, 1, axis=0)[0].astype(jnp.float32)
    sent = [
        lax.dynamic_slice_in_dim(pair, (z + d) % chips, 1, axis=0)[0] for d in range(1, chips)
    ]
    for d in range(1, chips):
        total = total + shift(sent[d - 1], d, size).astype(jnp.float32)
    return total.astype(jnp.bfloat16), sent


def tp_gather(value):
    return lax.all_gather(value, "tp", axis=0, tiled=True)


def tp_scatter(value):
    return lax.psum_scatter(value, "tp", scatter_dimension=0, tiled=True)


def body4(
    n_tp,
    later_tokens,
    earlier_tokens,
    earlier_cotangent,
    gate_weight,
    up_weight,
    down_weight,
    gate_sum,
    up_sum,
    down_sum,
):
    bf16 = jnp.bfloat16
    me = lax.axis_index("fs")
    e_tok = tp_gather(reorder(earlier_tokens, me))
    e_cot = tp_gather(reorder(earlier_cotangent, me))
    l_tok = tp_gather(after(reorder(later_tokens, me), e_tok))

    g1, g2 = near(gate_weight)
    u1, u2 = near(up_weight)
    g3 = far(g1, g2)
    d1, d2 = near(after(down_weight, g1, g2))
    u3 = far(u1, u2)
    d3 = far(d1, d2)
    gate_w = jnp.concatenate([gate_weight, g1, g2, *g3], axis=0)
    up_w = jnp.concatenate([up_weight, u1, u2, *u3], axis=0)
    down_w = jnp.concatenate(
        [down_weight, d1, d2, jnp.concatenate(d3, axis=0)], axis=1
    )

    earlier_gate = dot(e_tok, gate_w)
    earlier_up = dot(e_tok, up_w)
    s, act = silu_parts(earlier_gate)
    earlier_hidden = (act * earlier_up).astype(bf16)

    size = e_cot.shape[1] // 4
    down_blocks = [
        rows_dot(earlier_hidden, e_cot[:, j * size : (j + 1) * size]).astype(bf16)
        for j in range(4)
    ]
    down_got = scatter_start(down_blocks)

    hidden_grad = transposed_dot(e_cot, down_w)
    slope = s * (1.0 + earlier_gate * (1.0 - s))
    gate_grad = (hidden_grad * earlier_up * slope).astype(bf16)
    up_grad = (hidden_grad * act).astype(bf16)

    gate_blocks = [
        rows_dot(e_tok[:, j * size : (j + 1) * size], gate_grad).astype(bf16) for j in range(4)
    ]
    up_blocks = [
        rows_dot(e_tok[:, j * size : (j + 1) * size], up_grad).astype(bf16) for j in range(4)
    ]
    gate_got = scatter_start(gate_blocks)
    up_got = scatter_start(up_blocks)

    earlier_grad = tp_scatter(
        (transposed_dot(gate_grad, gate_w) + transposed_dot(up_grad, up_w)).astype(bf16)
    )
    l_tok = after(l_tok, *gate_blocks)
    later_hidden = (jax.nn.silu(dot(l_tok, gate_w)) * dot(l_tok, up_w)).astype(bf16)
    later_partial = dot(later_hidden, down_w).astype(bf16)
    later_output, sent = group_scatter(later_partial, n_tp)
    down_got, gate_got, up_got = (
        lax.optimization_barrier((*got, *sent))[:4] for got in (down_got, gate_got, up_got)
    )
    down_sum = after(down_sum, later_output)
    down_total = down_sum + scatter_end(down_blocks, down_got)
    gate_total = gate_sum + scatter_end(gate_blocks, gate_got)
    up_total = up_sum + scatter_end(up_blocks, up_got)
    return (reorder(later_output, me), reorder(earlier_grad, me), gate_total, up_total, down_total)


def body(
    later_tokens,
    earlier_tokens,
    earlier_cotangent,
    gate_weight,
    up_weight,
    down_weight,
    gate_sum,
    up_sum,
    down_sum,
):
    width = gate_weight.shape[1]
    gate_w, up_w, down_w = (
        lax.all_gather(gate_weight, "fs", axis=0, tiled=True),
        lax.all_gather(up_weight, "fs", axis=0, tiled=True),
        lax.all_gather(down_weight, "fs", axis=1, tiled=True),
    )
    piece = tp_gather(later_tokens)
    later_hidden = (jax.nn.silu(dot(piece, gate_w)) * dot(piece, up_w)).astype(jnp.bfloat16)
    later_output = tp_scatter(dot(later_hidden, down_w).astype(jnp.bfloat16))
    group_tokens, group_cotangent = tp_gather(earlier_tokens), tp_gather(earlier_cotangent)
    earlier_gate = dot(group_tokens, gate_w)
    earlier_up = dot(group_tokens, up_w)
    s, act = silu_parts(earlier_gate)
    earlier_hidden = (act * earlier_up).astype(jnp.bfloat16)
    hidden_grad = transposed_dot(group_cotangent, down_w)
    slope = s * (1.0 + earlier_gate * (1.0 - s))
    gate_grad = (hidden_grad * earlier_up * slope).astype(jnp.bfloat16)
    up_grad = (hidden_grad * act).astype(jnp.bfloat16)
    earlier_grad = tp_scatter(
        (transposed_dot(gate_grad, gate_w) + transposed_dot(up_grad, up_w)).astype(jnp.bfloat16)
    )
    summed = lax.psum_scatter(
        jnp.concatenate(
            [
                rows_dot(group_tokens, gate_grad),
                rows_dot(group_tokens, up_grad),
                rows_dot(group_cotangent, earlier_hidden),
            ],
            axis=1,
        ).astype(jnp.bfloat16),
        "fs",
        scatter_dimension=0,
        tiled=True,
    ).astype(jnp.float32)
    gate_total = gate_sum + summed[:, :width]
    up_total = up_sum + summed[:, width : 2 * width]
    down_total = down_sum + summed[:, 2 * width :].T
    return (later_output, earlier_grad, gate_total, up_total, down_total)


def solution(mesh):
    return jax.shard_map(
        functools.partial(body4, mesh.shape["tp"]) if mesh.shape["fs"] == 4 else body,
        mesh=mesh,
        in_specs=(
            P(("fs", "tp"), None),
            P(("fs", "tp"), None),
            P(("fs", "tp"), None),
            P("fs", "tp"),
            P("fs", "tp"),
            P("tp", "fs"),
            P("fs", "tp"),
            P("fs", "tp"),
            P("tp", "fs"),
        ),
        out_specs=(
            P(("fs", "tp"), None),
            P(("fs", "tp"), None),
            P("fs", "tp"),
            P("fs", "tp"),
            P("tp", "fs"),
        ),
        check_vma=False,
    )
```
